32 devices in a mesh: ep: 16 (over z, y, x), tp: 2 (over core).
Axes of the slice: x: 2, y: 2, z: 4, core: 2. Of those that a mesh axis runs over, the one named last changes fastest.
Arguments:
- tokens: bfloat16 [256, 2048], P('ep'), may hold values from -6 to 6
- state: float32 [256, 8, 128, 128], P('ep', 'tp'), may hold values from -6 to 6
- mix_gain: float32 [2048], replicated, may hold values from 0.1 to 1.9
- moe_gain: float32 [2048], replicated, may hold values from 0.1 to 1.9
- head_gain: float32 [128], replicated, may hold values from 0.1 to 1.9
- w_forget: bfloat16 [2048, 1024], P(None, 'tp'), may hold values from -0.125 to 0.125
- w_query: bfloat16 [2048, 1024], P(None, 'tp'), may hold values from -0.125 to 0.125
- w_input: bfloat16 [2048, 1024], P(None, 'tp'), may hold values from -0.125 to 0.125
- w_outgate: bfloat16 [2048, 1024], P(None, 'tp'), may hold values from -0.125 to 0.125
- lower_bound: float32 [1024], P('tp'), may hold values from 0 to 0.9
- w_mix_out: bfloat16 [1024, 2048], P('tp'), may hold values from -0.1875 to 0.1875
- routes: int32 [256, 6], P('ep'), may hold values from 0 to 15, all different within a row; in each aligned block of 16 rows (0 to 15, 16 to 31, ...) at most 16 rows name the same one
- route_scores: float32 [256, 6], P('ep'), may hold values from 0.05 to 1
- expert_gate: bfloat16 [16, 2048, 512], P('ep', None, 'tp'), may hold values from -0.125 to 0.125
- expert_up: bfloat16 [16, 2048, 512], P('ep', None, 'tp'), may hold values from -0.125 to 0.125
- expert_down: bfloat16 [16, 512, 2048], P('ep', 'tp'), may hold values from -0.25 to 0.25
- shared_gate: bfloat16 [2048, 512], P(None, 'tp'), may hold values from -0.125 to 0.125
- shared_up: bfloat16 [2048, 512], P(None, 'tp'), may hold values from -0.125 to 0.125
- shared_down: bfloat16 [512, 2048], P('tp'), may hold values from -0.25 to 0.25
Outputs:
- layer_out: bfloat16 [256, 2048], P('ep', 'tp')
- new_state: float32 [256, 8, 128, 128], P('ep', 'tp')
The draws below stay inside these ranges and needn't reach their ends.
Inputs may be any that keep to these rules, and one draw needn't show every extreme that they name: `routes`: each token names 6 different experts. Among the tokens of one index of ep no expert is named by more than 16 tokens, and in every draw some expert is named by exactly 16 tokens of some index of ep.
All inputs are finite; a program needn't handle non-finite values.
Results may differ from the reference program's by a relative error of at most 0.017.
Values may be sent and summed in bfloat16 or wider, within the bound.
A program may use at most 128 MiB of HBM per device.

```python
import math
import jax
import jax.numpy as jnp
import numpy as np
from jax import lax

D = 2048
HEADS = 8
HEAD_KEY = 128
HEAD_VALUE = 128
FE = 512
TOP_K = 6
S_DEV = 16
EXPERTS = 16
SEQS = 256
CAP = 16
N_EP = 16


def steps_of(own_key, shape, pieces, smallest, largest):
    level = 1.0
    for position, parts in pieces:
        draws = jax.random.uniform(jax.random.fold_in(jax.random.fold_in(own_key, 6), position), (parts,), jnp.float32, smallest / len(pieces), largest / len(pieces))
        level = level * jnp.repeat(jnp.exp(draws), shape[position] // parts).reshape((-1,) + (1,) * (len(shape) - 1 - position))
    return level


def deal_out(own_key, own, number, rows, number_of, top, bound, slope):
    order = jax.random.permutation(own_key, number_of)
    heavy_load, usual = shares(number_of, rows * top, bound, slope, True), shares(number_of, rows * top, bound, slope, False)
    places = jnp.arange(number_of)

    def named(sizes, offset_by):
        used = int((sizes > 0).sum())
        fixed = max(1, used // 4)
        moved = fixed + (places - fixed + offset_by * (used - fixed)) % max(1, number_of - fixed)
        return jnp.zeros((number_of,), jnp.int32).at[order[jnp.where(places < fixed, places, moved)]].set(jnp.asarray(sizes, jnp.int32))

    sizes = jnp.where(number % 4 == 0, named(heavy_load, number // 4), named(usual, number - number // 4 - 1))
    mixed = jax.random.permutation(jax.random.fold_in(own, 3), number_of)
    giver, taker = mixed[0:number_of // 2 * 2:2], mixed[1:number_of // 2 * 2:2]
    margin = jnp.minimum(sizes[giver] - 1, bound - sizes[taker]) // 2
    margin = jnp.where((giver == order[0]) | (taker == order[0]) | (sizes[taker] == 0), 0, jnp.maximum(margin, 0))
    moved = jax.random.randint(jax.random.fold_in(own, 4), (number_of // 2,), 0, 1 << 20) % (margin + 1)
    sizes = sizes.at[giver].add(-moved).at[taker].add(moved)
    items = jnp.searchsorted(jnp.cumsum(sizes), jnp.arange(rows * top), side="right").astype(jnp.int32)
    grid = items.reshape(top, rows).T
    grid = grid[jax.random.permutation(jax.random.fold_in(own, 1), rows)]
    offset_by = jax.random.randint(jax.random.fold_in(own, 2), (rows, 1), 0, top)
    return jnp.take_along_axis(grid, (jnp.arange(top)[None, :] + offset_by) % top, axis=1)


def shares(number_of, total, most, slope, full):
    loads = [(1 << 20) // math.isqrt(standing ** slope) + 1 for standing in range(1, number_of + 1)]
    largest = most if full else min(most, max(-(-total // number_of), total * loads[0] // sum(loads)))
    least = 1 if total - largest >= number_of - 1 else 0
    counts, spare = [largest] + [least] * (number_of - 1), total - largest - least * (number_of - 1)
    while spare > 0:
        movable = [i for i in range(1, number_of) if counts[i] < largest] or [i for i in range(1, number_of) if counts[i] < most]
        mass, remaining = sum([loads[i] for i in movable]), spare
        for i in movable:
            extra = min(most - counts[i], max(1, remaining * loads[i] // mass), spare)
            counts[i] = counts[i] + extra
            spare = spare - extra
    return np.array(counts)


def centred(stream_key, shape, deviation, bound, shards=(), kind=jnp.bfloat16):
    array = jax.random.normal(stream_key, shape, jnp.float32) * deviation
    if len(shards) > 0:
        array = steps_of(stream_key, shape, shards, -0.22, 0.18) * array
    return jnp.clip(array, min=-bound, max=bound).astype(kind)


def setup_inputs(seed: int = 0) -> dict:
    keys = jax.random.split(jax.random.key(seed), 20)
    tokens = centred(keys[0], (SEQS, D), 1.0, 6.0, ((0, 16),))
    state = centred(keys[1], (SEQS, HEADS, HEAD_KEY, HEAD_VALUE), 1.0, 6.0, ((0, 16), (1, 2)), jnp.float32)
    mix_gain = jnp.clip(1.0 + 0.18 * jax.random.normal(keys[2], (D,), jnp.float32), 0.1, 1.9)
    moe_gain = jnp.clip(1.0 + 0.18 * jax.random.normal(keys[3], (D,), jnp.float32), 0.1, 1.9)
    head_gain = jnp.clip(1.0 + 0.18 * jax.random.normal(keys[4], (HEAD_VALUE,), jnp.float32), 0.1, 1.9)
    w_forget = centred(keys[5], (D, HEADS * HEAD_KEY), D ** -0.5, 0.125, ((1, 2),))
    w_query = centred(keys[6], (D, HEADS * HEAD_KEY), D ** -0.5, 0.125, ((1, 2),))
    w_input = centred(keys[7], (D, HEADS * HEAD_VALUE), D ** -0.5, 0.125, ((1, 2),))
    w_outgate = centred(keys[8], (D, HEADS * HEAD_VALUE), D ** -0.5, 0.125, ((1, 2),))
    lower_bound = jnp.clip(0.9 * jax.random.uniform(keys[9], (HEADS * HEAD_KEY,), jnp.float32) ** steps_of(keys[9], (HEADS * HEAD_KEY,), ((0, 2),), -0.2, 0.2), 0.0, 0.9)
    w_mix_out = centred(keys[10], (HEADS * HEAD_VALUE, D), (HEADS * HEAD_VALUE) ** -0.5, 0.1875, ((0, 2),))
    routes_keys = jax.random.split(jax.random.fold_in(keys[11], 1), SEQS // S_DEV)
    routes_turns = jax.random.permutation(jax.random.fold_in(keys[11], 3), SEQS // S_DEV)
    routes = jax.vmap(lambda own, number: deal_out(jax.random.fold_in(keys[11], 2), own, number, S_DEV, EXPERTS, TOP_K, CAP, 2))(routes_keys, routes_turns).reshape((SEQS, TOP_K))
    route_scores = jnp.clip(0.05 + 0.95 * jax.random.uniform(keys[12], (SEQS, TOP_K), jnp.float32) ** steps_of(keys[12], (SEQS, TOP_K), ((0, 16),), -0.2, 0.2), 0.05, 1.0)
    expert_gate = centred(keys[13], (EXPERTS, D, FE), D ** -0.5, 0.125, ((0, 16), (2, 2)))
    expert_up = centred(keys[14], (EXPERTS, D, FE), D ** -0.5, 0.125, ((0, 16), (2, 2)))
    expert_down = centred(keys[15], (EXPERTS, FE, D), FE ** -0.5, 0.25, ((0, 16), (1, 2)))
    shared_gate = centred(keys[16], (D, FE), D ** -0.5, 0.125, ((1, 2),))
    shared_up = centred(keys[17], (D, FE), D ** -0.5, 0.125, ((1, 2),))
    shared_down = centred(keys[18], (FE, D), FE ** -0.5, 0.25, ((0, 2),))
    return dict(tokens=tokens, state=state, mix_gain=mix_gain, moe_gain=moe_gain, head_gain=head_gain, w_forget=w_forget, w_query=w_query, w_input=w_input, w_outgate=w_outgate, lower_bound=lower_bound, w_mix_out=w_mix_out, routes=routes, route_scores=route_scores, expert_gate=expert_gate, expert_up=expert_up, expert_down=expert_down, shared_gate=shared_gate, shared_up=shared_up, shared_down=shared_down)


epsilon = 1e-06
routed_scale = 2.5

def rms_scale(values, gain):
    return values * lax.rsqrt(lax.optimization_barrier(jnp.mean(values * values, axis=-1, keepdims=True)) + epsilon) * gain

def rounded(values):
    return lax.optimization_barrier(values.astype(jnp.bfloat16)).astype(jnp.float32)

def halves_sum(operand, weight, split_at):
    first = jnp.dot(operand[:, :split_at], weight[:split_at], preferred_element_type=jnp.float32)
    second = jnp.dot(operand[:, split_at:], weight[split_at:], preferred_element_type=jnp.float32)
    return (rounded(first) + rounded(second)).astype(jnp.bfloat16)

def reference(tokens, state, mix_gain, moe_gain, head_gain, w_forget, w_query, w_input, w_outgate, lower_bound, w_mix_out, routes, route_scores, expert_gate, expert_up, expert_down, shared_gate, shared_up, shared_down):
    seq_count = tokens.shape[0]
    tokens_wide = tokens.astype(jnp.float32)
    normed = rms_scale(tokens_wide, mix_gain).astype(jnp.bfloat16)
    forget_pre = jnp.dot(normed, w_forget, preferred_element_type=jnp.float32).reshape(seq_count, HEADS, HEAD_KEY)
    query = jax.nn.silu(jnp.dot(normed, w_query, preferred_element_type=jnp.float32)).reshape(seq_count, HEADS, HEAD_KEY)
    input_val = jnp.dot(normed, w_input, preferred_element_type=jnp.float32).reshape(seq_count, HEADS, HEAD_VALUE)
    gate_pre = jnp.dot(normed, w_outgate, preferred_element_type=jnp.float32).reshape(seq_count, HEADS, HEAD_VALUE)
    bound_rows = lower_bound.reshape(HEADS, HEAD_KEY)
    forget = bound_rows + (1.0 - bound_rows) * jax.nn.sigmoid(forget_pre)
    key_gate = (1.0 - bound_rows) * jax.nn.sigmoid(-forget_pre)
    new_state = forget[..., None] * state + key_gate[..., None] * input_val[:, :, None, :]
    readout = jnp.einsum('shkv,shk->shv', new_state, query, precision=lax.Precision.HIGHEST)
    gated_out = (rms_scale(readout, head_gain) * jax.nn.silu(gate_pre)).astype(jnp.bfloat16)
    gated_out = gated_out.reshape(seq_count, HEADS * HEAD_VALUE)
    mixer_out = halves_sum(gated_out, w_mix_out, HEADS * HEAD_VALUE // 2)
    residual = tokens_wide + mixer_out.astype(jnp.float32)
    moe_rows = rms_scale(residual, moe_gain).astype(jnp.bfloat16)
    weights = route_scores / lax.optimization_barrier(jnp.sum(route_scores, axis=-1, keepdims=True)) * routed_scale
    shared_hidden = (jax.nn.silu(jnp.dot(moe_rows, shared_gate, preferred_element_type=jnp.float32)) * jnp.dot(moe_rows, shared_up, preferred_element_type=jnp.float32)).astype(jnp.bfloat16)
    shared_out = halves_sum(shared_hidden, shared_down, FE // 2)
    flat_routes = routes.reshape(-1)
    slot_count = N_EP * CAP
    rows_repeated = jnp.repeat(moe_rows, TOP_K, axis=0)

    def one_expert(totals, inputs):
        gate_w, up_w, down_w, expert_id = inputs
        chosen = flat_routes == expert_id
        slot_rank = (jnp.cumsum(chosen.astype(jnp.int32)) - 1).astype(jnp.int32)
        target = jnp.where(chosen, slot_rank, slot_count).astype(jnp.int32)
        buffer = jnp.zeros((slot_count, D), jnp.bfloat16).at[target].set(rows_repeated, mode='drop')
        hidden = (jax.nn.silu(jnp.dot(buffer, gate_w, preferred_element_type=jnp.float32)) * jnp.dot(buffer, up_w, preferred_element_type=jnp.float32)).astype(jnp.bfloat16)
        result = halves_sum(hidden, down_w, FE // 2)
        picked = result[jnp.clip(slot_rank, 0, slot_count - 1)].astype(jnp.float32)
        return (totals + jnp.where(chosen[:, None], picked, jnp.float32(0.0)), None)
    totals, _ = lax.scan(one_expert, jnp.zeros((seq_count * TOP_K, D), jnp.float32), (expert_gate, expert_up, expert_down, jnp.arange(EXPERTS, dtype=jnp.int32)))
    routed = lax.optimization_barrier(jnp.sum(totals.reshape(seq_count, TOP_K, D) * weights[:, :, None], axis=1))
    layer_out = (residual + routed + shared_out.astype(jnp.float32)).astype(jnp.bfloat16)
    return (layer_out, new_state)
```

```python
import functools

import jax
import jax.numpy as jnp
from jax import lax
from jax.experimental import pallas as pl
from jax.experimental.pallas import tpu as pltpu
from jax.sharding import PartitionSpec as P

epsilon = 1e-06
routed_scale = 2.5
MESH = pl.DeviceIdType.MESH
f32 = jnp.float32
bf16 = jnp.bfloat16


def dot(a, b):
    return jnp.dot(a, b, preferred_element_type=f32)


def silu(v):
    return v * jax.nn.sigmoid(v)


def rms_scale(values, gain):
    return values * lax.rsqrt(jnp.mean(values * values, axis=-1, keepdims=True) + epsilon) * gain


def mixer_kernel(
    tok, gain, head_gain, bound, routes, scores, wf, wi, wq, wg, wm, st,
    partial, weights_out, new_st,
    wbuf, wmbuf, sbuf, nbuf, readout, gated, wsem, ssem, osem,
):
    seqs, heads, kdim, vdim = st.shape
    copies = [
        pltpu.make_async_copy(w, wbuf.at[i], wsem.at[i]) for i, w in enumerate((wf, wi, wq, wg))
    ]
    mix_copy = pltpu.make_async_copy(wm, wmbuf, wsem.at[4])
    state_copies = [
        pltpu.make_async_copy(st.at[:, h], sbuf.at[h], ssem.at[h]) for h in range(heads)
    ]
    for c in copies[:3] + state_copies + copies[3:] + [mix_copy]:
        c.start()
    normed = rms_scale(tok[...].astype(f32), gain[...]).astype(bf16)

    score = scores[...]
    top = score.shape[1]
    weight = score / jnp.sum(score, axis=-1, keepdims=True) * routed_scale
    named = routes[...]
    experts = weights_out.shape[0]
    wide = -(-experts // 128) * 128
    lane = lax.broadcasted_iota(jnp.int32, (seqs, wide), 1)
    dense = jnp.zeros((seqs, wide), f32)
    for t in range(top):
        dense += jnp.where(named[:, t : t + 1] == lane, weight[:, t : t + 1], 0.0)
    tall = weights_out.shape[2]
    dense = jnp.concatenate([dense, jnp.zeros((tall - seqs, wide), f32)], axis=0)
    weights_out[:, 0, :] = dense.T[:experts]

    copies[0].wait()
    forget_pre = dot(normed, wbuf[0])
    low = bound[...]
    forget = low + (1.0 - low) * jax.nn.sigmoid(forget_pre)
    key = (1.0 - low) * jax.nn.sigmoid(-forget_pre)
    copies[1].wait()
    value = dot(normed, wbuf[1])
    copies[2].wait()
    query = silu(dot(normed, wbuf[2]))
    outs = []
    for h in range(heads):
        cols = slice(h * kdim, (h + 1) * kdim)
        vcols = slice(h * vdim, (h + 1) * vdim)
        ft, kt, qt = forget[:, cols].T, key[:, cols].T, query[:, cols].T
        vh = value[:, vcols]
        state_copies[h].wait()
        for s in range(seqs):
            new = ft[:, s : s + 1] * sbuf[h, s] + kt[:, s : s + 1] * vh[s : s + 1]
            nbuf[h, s] = new
            readout[s : s + 1, vcols] = jnp.sum(new * qt[:, s : s + 1], axis=0, keepdims=True)
        out = pltpu.make_async_copy(nbuf.at[h], new_st.at[:, h], osem.at[h])
        out.start()
        outs.append(out)
    copies[3].wait()
    gate = silu(dot(normed, wbuf[3]))
    for h in range(heads):
        vcols = slice(h * vdim, (h + 1) * vdim)
        gated[:, vcols] = (
            rms_scale(readout[:, vcols], head_gain[...]) * gate[:, vcols]
        ).astype(bf16)
    mix_copy.wait()
    partial[...] = dot(gated[...], wmbuf[...]).astype(bf16)
    for out in outs:
        out.wait()


def moe_kernel(
    n_ep, n_z, tok, part_in, gain, wsrc, eg, eu, ed, sg, su, sd,
    out_ref,
    peer_part, rows, hidden, res, wgot, egb, eub, edb, sgb, sub, sdb,
    shared_send, shared_got, shared_mine, other, mine, cross, weighted, plane_got, line_send, line_got, scale_ref,
    wsem, bar_v_s, bar_v_r, ps_s, ps_r, a1_s, a1_r, a2_s, a2_r, fw_s, fw_r,
    sh_s, sh_r, x_s, x_r, g_s, g_r, l_s, l_r,
):
    n_p = n_ep // n_z
    me = lax.axis_index("ep")
    tp = lax.axis_index("tp")
    mate = 1 - tp
    z = me // n_p
    q = me % n_p
    seqs, width = tok.shape
    half = width // 2
    barrier = pltpu.get_barrier_semaphore()
    pl.semaphore_signal(barrier, inc=1, device_id=(me, mate), device_id_type=MESH)
    for k in range(1, n_ep):
        pl.semaphore_signal(
            barrier, inc=1, device_id=((me + k) % n_ep, tp), device_id_type=MESH
        )
    loads = []
    pairs = [(sg, sgb), (su, sub), (eg.at[0], egb), (eu.at[0], eub)]
    for i, (src, dst) in enumerate(pairs):
        loads.append(pltpu.make_async_copy(src, dst, wsem.at[i]))
    for c in range(2):
        loads.append(
            pltpu.make_async_copy(sd.at[:, pl.ds(c * half, half)], sdb.at[c], wsem.at[4 + c])
        )
        loads.append(
            pltpu.make_async_copy(ed.at[0, :, pl.ds(c * half, half)], edb.at[c], wsem.at[6 + c])
        )
    for c in loads:
        c.start()
    pl.semaphore_wait(barrier, n_ep)

    def send(src, dst, s, r, ep, core):
        c = pltpu.make_async_remote_copy(
            src_ref=src, dst_ref=dst, send_sem=s, recv_sem=r,
            device_id=(ep, core), device_id_type=MESH,
        )
        c.start()
        return c

    started = []
    psum = send(part_in, peer_part, ps_s, ps_r, me, mate)
    for k in range(1, n_ep):
        to = (me + k) % n_ep
        started.append(send(wsrc.at[to], wgot.at[me], bar_v_s.at[k], bar_v_r.at[k], to, tp))
    weight_copies = started[:]
    psum.wait()
    mixed = (part_in[...].astype(f32) + peer_part[...].astype(f32)).astype(bf16)
    residual = tok[...].astype(f32) + mixed.astype(f32)
    normed = rms_scale(residual, gain[...]).astype(bf16)
    own = pl.ds(pl.multiple_of(me * seqs, seqs), seqs)
    for c in range(2):
        cols = slice(c * half, (c + 1) * half)
        rows[c, own] = normed[:, cols]
        res[c] = residual[:, cols]

    def block(j):
        return rows.at[tp, pl.ds(pl.multiple_of(j * seqs, seqs), seqs)]

    line = [None]
    for d in range(1, n_z):
        to = (z + d) % n_z * n_p + q
        line.append(send(block(me), block(me), a1_s.at[d], a1_r.at[d], to, tp))
    plane = {}

    def to_plane(d):
        j = (z + n_z - d) % n_z * n_p + q
        for k in range(1, n_p):
            to = z * n_p + (q + k) % n_p
            plane[d, k] = send(
                block(j), block(j), a2_s.at[d * n_p + k], a2_r.at[d * n_p + k], to, tp
            )

    forwards = []

    def to_mate(d, k):
        j = (z + n_z - d) % n_z * n_p + (q + n_p - k) % n_p
        i = d * n_p + k
        forwards.append(send(block(j), block(j), fw_s.at[i], fw_r.at[i], me, mate))

    to_plane(0)

    loads[0].wait()
    loads[1].wait()
    shared_hidden = (silu(dot(normed, sgb[...])) * dot(normed, sub[...])).astype(bf16)
    loads[4].wait()
    loads[6].wait()
    shared_send[...] = dot(shared_hidden, sdb[mate]).astype(bf16)
    shared_copy = send(shared_send, shared_got, sh_s, sh_r, me, mate)
    shared_mine[...] = dot(shared_hidden, sdb[tp]).astype(bf16)

    for d in range(1, n_z):
        line[d].wait_recv()
        to_plane(d)
        to_mate(d, 0)
    for d in range(n_z):
        for k in range(1, n_p):
            plane[d, k].wait_recv()
            to_mate(d, k)

    for k in range(1, n_ep):
        weight_copies[k - 1].wait_recv()
    wgot[me] = wsrc[me]
    tall = wgot.shape[2]
    spread = jnp.broadcast_to(wgot[...], (n_ep, seqs, tall))
    at_lane = lax.broadcasted_iota(jnp.int32, (n_ep, seqs, tall), 2)
    at_row = lax.broadcasted_iota(jnp.int32, (n_ep, seqs, tall), 1)
    column = jnp.sum(jnp.where(at_lane == at_row, spread, 0.0), axis=2, keepdims=True)
    column = column.reshape(n_ep * seqs, 1)
    loads[2].wait()
    loads[3].wait()
    loads[5].wait()
    loads[7].wait()
    for f in forwards:
        f.wait_recv()
    left, right = rows[0], rows[1]
    gate = dot(left, egb[:half]) + dot(right, egb[half:])
    up = dot(left, eub[:half]) + dot(right, eub[half:])
    hidden[...] = (silu(gate) * up).astype(bf16)
    scale = jnp.broadcast_to(column, (n_ep * seqs, 128))

    chunk = n_p * seqs
    order = list(range(1, n_z)) + [0]
    crossing = {}
    scale_ref[...] = scale
    for d in order:
        at = pl.ds(pl.multiple_of((z + d) % n_z * chunk, chunk), chunk)
        h = hidden[at]
        other[d] = dot(h, edb[mate]).astype(bf16)
        crossing[d] = send(other.at[d], cross.at[d], x_s.at[d], x_r.at[d], me, mate)
        mine[d] = dot(h, edb[tp]).astype(bf16)
    returns = {}
    for d in order:
        at = pl.ds(pl.multiple_of((z + d) % n_z * chunk, chunk), chunk)
        crossing[d].wait_recv()
        whole = (mine[d].astype(f32) + cross[d].astype(f32)).astype(bf16).astype(f32)
        weighted[d] = (whole * scale_ref[at, 0:1]).astype(bf16)
        for k in range(1, n_p):
            to = (q + k) % n_p
            src = weighted.at[d, pl.ds(pl.multiple_of(to * seqs, seqs), seqs)]
            i = d * n_p + k
            returns[d, k] = send(src, plane_got.at[i], g_s.at[i], g_r.at[i], z * n_p + to, tp)
    mine_at = pl.ds(pl.multiple_of(q * seqs, seqs), seqs)
    lines = {}
    total = None
    for d in order:
        total = weighted[d, mine_at].astype(f32)
        for k in range(1, n_p):
            returns[d, k].wait_recv()
            total += plane_got[d * n_p + k].astype(f32)
        if d > 0:
            sums = line_send.at[d]
            line_send[d] = total.astype(bf16)
            lines[d] = send(
                sums, line_got.at[d], l_s.at[d], l_r.at[d], (z + d) % n_z * n_p + q, tp
            )
    shared_copy.wait_recv()
    shared = (shared_mine[...].astype(f32) + shared_got[...].astype(f32)).astype(bf16)
    for d in range(1, n_z):
        lines[d].wait_recv()
        total += line_got[d].astype(f32)
    out_ref[...] = (res[tp] + total + shared.astype(f32)).astype(bf16)
    everything = started + line[1:] + list(plane.values()) + forwards
    everything += list(crossing.values()) + list(returns.values()) + list(lines.values())
    for c in everything + [shared_copy]:
        c.wait_send()


def local(n_ep, *args):
    (
        tokens, state, mix_gain, moe_gain, head_gain, w_forget, w_query, w_input, w_outgate,
        lower_bound, w_mix_out, routes, route_scores, expert_gate, expert_up, expert_down,
        shared_gate, shared_up, shared_down,
    ) = args
    seqs, width = tokens.shape
    heads, kdim, vdim = state.shape[1:]
    half = width // 2
    n_z = max(d for d in range(1, n_ep + 1) if d * d <= n_ep and n_ep % d == 0)
    n_p = n_ep // n_z
    experts = expert_gate.shape[0] * n_ep
    tall = -(-seqs // 128) * 128
    vmem = pl.BlockSpec(memory_space=pltpu.VMEM)
    anym = pl.BlockSpec(memory_space=pl.ANY)
    dma = pltpu.SemaphoreType.DMA
    inner = heads * vdim
    partial, dense, new_state = pl.pallas_call(
        mixer_kernel,
        out_shape=(
            jax.ShapeDtypeStruct((seqs, width), bf16),
            jax.ShapeDtypeStruct((experts, 1, tall), f32),
            jax.ShapeDtypeStruct(state.shape, f32),
        ),
        in_specs=[vmem] * 6 + [anym] * 6,
        out_specs=(vmem, vmem, anym),
        scratch_shapes=[
            pltpu.VMEM((4,) + w_forget.shape, bf16),
            pltpu.VMEM(w_mix_out.shape, bf16),
            pltpu.VMEM((heads, seqs, kdim, vdim), f32),
            pltpu.VMEM((heads, seqs, kdim, vdim), f32),
            pltpu.VMEM((seqs, inner), f32),
            pltpu.VMEM((seqs, inner), bf16),
            dma((5,)),
            dma((heads,)),
            dma((heads,)),
        ],
        name="mixer",
    )(
        tokens, mix_gain.reshape(1, -1), head_gain.reshape(1, -1), lower_bound.reshape(1, -1),
        routes, route_scores, w_forget, w_input, w_query, w_outgate, w_mix_out, state,
    )
    hid = expert_gate.shape[2]
    shid = shared_gate.shape[1]
    chunk = n_p * seqs
    layer_out = pl.pallas_call(
        functools.partial(moe_kernel, n_ep, n_z),
        out_shape=jax.ShapeDtypeStruct((seqs, half), bf16),
        in_specs=[vmem] * 4 + [anym] * 6,
        out_specs=vmem,
        scratch_shapes=[
            pltpu.VMEM((seqs, width), bf16),
            pltpu.VMEM((2, n_ep * seqs, half), bf16),
            pltpu.VMEM((n_ep * seqs, hid), bf16),
            pltpu.VMEM((2, seqs, half), f32),
            pltpu.VMEM((n_ep, 1, tall), f32),
            pltpu.VMEM((width, hid), bf16),
            pltpu.VMEM((width, hid), bf16),
            pltpu.VMEM((2, hid, half), bf16),
            pltpu.VMEM((width, shid), bf16),
            pltpu.VMEM((width, shid), bf16),
            pltpu.VMEM((2, shid, half), bf16),
            pltpu.VMEM((seqs, half), bf16),
            pltpu.VMEM((seqs, half), bf16),
            pltpu.VMEM((seqs, half), bf16),
            pltpu.VMEM((n_z, chunk, half), bf16),
            pltpu.VMEM((n_z, chunk, half), bf16),
            pltpu.VMEM((n_z, chunk, half), bf16),
            pltpu.VMEM((n_z, chunk, half), bf16),
            pltpu.VMEM((n_ep, seqs, half), bf16),
            pltpu.VMEM((n_z, seqs, half), bf16),
            pltpu.VMEM((n_z, seqs, half), bf16),
            pltpu.VMEM((n_ep * seqs, 128), f32),
            dma((8,)),
            dma((n_ep,)), dma((n_ep,)),
            dma, dma,
            dma((n_z,)), dma((n_z,)),
            dma((n_ep,)), dma((n_ep,)),
            dma((n_ep,)), dma((n_ep,)),
            dma, dma,
            dma((n_z,)), dma((n_z,)),
            dma((n_ep,)), dma((n_ep,)),
            dma((n_z,)), dma((n_z,)),
        ],
        compiler_params=pltpu.CompilerParams(collective_id=0, has_side_effects=True),
        name="experts",
    )(
        tokens, partial, moe_gain.reshape(1, -1), dense,
        expert_gate, expert_up, expert_down, shared_gate, shared_up, shared_down,
    )
    return (layer_out, new_state)


def solution(mesh):
    return jax.shard_map(
        functools.partial(local, mesh.shape["ep"]),
        mesh=mesh,
        in_specs=(
            P("ep", None),
            P("ep", "tp", None, None),
            P(),
            P(),
            P(),
            P(None, "tp"),
            P(None, "tp"),
            P(None, "tp"),
            P(None, "tp"),
            P("tp"),
            P("tp", None),
            P("ep", None),
            P("ep", None),
            P("ep", None, "tp"),
            P("ep", None, "tp"),
            P("ep", "tp", None),
            P(None, "tp"),
            P(None, "tp"),
            P("tp", None),
        ),
        out_specs=(P("ep", "tp"), P("ep", "tp", None, None)),
        check_vma=False,
    )
```

```python
import functools

import jax
import jax.numpy as jnp
from jax import lax
from jax.experimental import pallas as pl
from jax.experimental.pallas import tpu as pltpu
from jax.sharding import PartitionSpec as P

epsilon = 1e-06
routed_scale = 2.5
MESH = pl.DeviceIdType.MESH
f32 = jnp.float32
bf16 = jnp.bfloat16


def dot(a, b):
    return jnp.dot(a, b, preferred_element_type=f32)


def silu(v):
    return v * jax.nn.sigmoid(v)


def rms_scale(values, gain):
    return values * lax.rsqrt(jnp.mean(values * values, axis=-1, keepdims=True) + epsilon) * gain


def mixer_kernel(
    tok, gain, bound, routes, scores, wf, wi, wq, st,
    normed_out, readout, weights_out, new_st,
    wbuf, sbuf, nbuf, wsem, ssem, osem,
):
    seqs, heads, kdim, vdim = st.shape
    copies = [
        pltpu.make_async_copy(w, wbuf.at[i], wsem.at[i]) for i, w in enumerate((wf, wi, wq))
    ]
    state_copies = [
        pltpu.make_async_copy(st.at[:, h], sbuf.at[h], ssem.at[h]) for h in range(heads)
    ]
    for c in copies + state_copies:
        c.start()
    normed = rms_scale(tok[...].astype(f32), gain[...]).astype(bf16)
    normed_out[...] = normed

    score = scores[...]
    top = score.shape[0]
    weight = score / jnp.sum(score, axis=0, keepdims=True) * routed_scale
    named = routes[...]
    experts = weights_out.shape[0]
    number = lax.broadcasted_iota(jnp.int32, (experts, seqs), 0)
    dense = jnp.zeros((experts, seqs), f32)
    for t in range(top):
        dense += jnp.where(named[t : t + 1] == number, weight[t : t + 1], 0.0)
    tall = weights_out.shape[2]
    weights_out[:, 0, :] = jnp.concatenate([dense, jnp.zeros((experts, tall - seqs), f32)], axis=1)

    copies[0].wait()
    forget_pre = dot(normed, wbuf[0])
    low = bound[...]
    forget = low + (1.0 - low) * jax.nn.sigmoid(forget_pre)
    key = (1.0 - low) * jax.nn.sigmoid(-forget_pre)
    copies[1].wait()
    value = dot(normed, wbuf[1])
    copies[2].wait()
    query = silu(dot(normed, wbuf[2]))
    outs = []
    for h in range(heads):
        cols = slice(h * kdim, (h + 1) * kdim)
        vcols = slice(h * vdim, (h + 1) * vdim)
        ft, kt, qt = forget[:, cols].T, key[:, cols].T, query[:, cols].T
        vh = value[:, vcols]
        state_copies[h].wait()
        for s in range(seqs):
            new = ft[:, s : s + 1] * sbuf[h, s] + kt[:, s : s + 1] * vh[s : s + 1]
            nbuf[h, s] = new
            readout[s : s + 1, vcols] = jnp.sum(new * qt[:, s : s + 1], axis=0, keepdims=True)
        out = pltpu.make_async_copy(nbuf.at[h], new_st.at[:, h], osem.at[h])
        out.start()
        outs.append(out)
    for out in outs:
        out.wait()


def moe_kernel(
    n_ep, n_z, tok, mixer_in, readout, head_gain, gain, wsrc, wg, wm, eg, eu, ed, sg, su, sd,
    out_ref,
    wgb, wmb, gated, part_in, peer_part, rows, res, wgot, egb, eub, edb, sgb, sub, sdb,
    shared_send, shared_got, shared_mine, other, mine, cross, weighted, plane_got, line_send, line_got, scale_ref,
    wsem, bar_v_s, bar_v_r, ps_s, ps_r, a1_s, a1_r, a2_s, a2_r, fw_s, fw_r,
    sh_s, sh_r, x_s, x_r, g_s, g_r, l_s, l_r,
):
    n_p = n_ep // n_z
    me = lax.axis_index("ep")
    tp = lax.axis_index("tp")
    mate = 1 - tp
    z = me // n_p
    q = me % n_p
    seqs, width = tok.shape
    half = width // 2
    barrier = pltpu.get_barrier_semaphore()
    pl.semaphore_signal(barrier, inc=1, device_id=(me, mate), device_id_type=MESH)
    for k in range(1, n_ep):
        pl.semaphore_signal(
            barrier, inc=1, device_id=((me + k) % n_ep, tp), device_id_type=MESH
        )
    gate_load = pltpu.make_async_copy(wg, wgb, wsem.at[8])
    mix_load = pltpu.make_async_copy(wm, wmb, wsem.at[9])
    gate_load.start()
    mix_load.start()
    loads = []
    pairs = [(sg, sgb), (su, sub), (eg.at[0], egb), (eu.at[0], eub)]
    for i, (src, dst) in enumerate(pairs):
        loads.append(pltpu.make_async_copy(src, dst, wsem.at[i]))
    for c in range(2):
        loads.append(
            pltpu.make_async_copy(sd.at[:, pl.ds(c * half, half)], sdb.at[c], wsem.at[4 + c])
        )
        loads.append(
            pltpu.make_async_copy(ed.at[0, :, pl.ds(c * half, half)], edb.at[c], wsem.at[6 + c])
        )
    for c in loads:
        c.start()
    gate_load.wait()
    open_gate = silu(dot(mixer_in[...], wgb[...]))
    vdim = head_gain.shape[1]
    for h in range(readout.shape[1] // vdim):
        vcols = slice(h * vdim, (h + 1) * vdim)
        gated[:, vcols] = (
            rms_scale(readout[:, vcols], head_gain[...]) * open_gate[:, vcols]
        ).astype(bf16)
    mix_load.wait()
    part_in[...] = dot(gated[...], wmb[...]).astype(bf16)
    pl.semaphore_wait(barrier, n_ep)

    def send(src, dst, s, r, ep, core):
        c = pltpu.make_async_remote_copy(
            src_ref=src, dst_ref=dst, send_sem=s, recv_sem=r,
            device_id=(ep, core), device_id_type=MESH,
        )
        c.start()
        return c

    started = []
    psum = send(part_in, peer_part, ps_s, ps_r, me, mate)
    for k in range(1, n_ep):
        to = (me + k) % n_ep
        started.append(send(wsrc.at[to], wgot.at[me], bar_v_s.at[k], bar_v_r.at[k], to, tp))
    weight_copies = started[:]
    psum.wait()
    mixed = (part_in[...].astype(f32) + peer_part[...].astype(f32)).astype(bf16)
    residual = tok[...].astype(f32) + mixed.astype(f32)
    normed = rms_scale(residual, gain[...]).astype(bf16)
    own = pl.ds(pl.multiple_of(me * seqs, seqs), seqs)
    for c in range(2):
        cols = slice(c * half, (c + 1) * half)
        rows[c, own] = normed[:, cols]
        res[c] = residual[:, cols]

    def block(j):
        return rows.at[tp, pl.ds(pl.multiple_of(j * seqs, seqs), seqs)]

    line = [None]
    for d in range(1, n_z):
        to = (z + d) % n_z * n_p + q
        line.append(send(block(me), block(me), a1_s.at[d], a1_r.at[d], to, tp))
    plane = {}

    def to_plane(d):
        j = (z + n_z - d) % n_z * n_p + q
        for k in range(1, n_p):
            to = z * n_p + (q + k) % n_p
            plane[d, k] = send(
                block(j), block(j), a2_s.at[d * n_p + k], a2_r.at[d * n_p + k], to, tp
            )

    forwards = {}

    def to_mate(d, k):
        j = (z + n_z - d) % n_z * n_p + (q + n_p - k) % n_p
        i = d * n_p + k
        forwards[d, k] = send(block(j), block(j), fw_s.at[i], fw_r.at[i], me, mate)

    to_plane(0)

    loads[0].wait()
    loads[1].wait()
    shared_hidden = (silu(dot(normed, sgb[...])) * dot(normed, sub[...])).astype(bf16)
    loads[4].wait()
    loads[6].wait()
    shared_send[...] = dot(shared_hidden, sdb[mate]).astype(bf16)
    shared_copy = send(shared_send, shared_got, sh_s, sh_r, me, mate)
    shared_mine[...] = dot(shared_hidden, sdb[tp]).astype(bf16)

    for d in range(1, n_z):
        line[d].wait_recv()
        to_plane(d)
        to_mate(d, 0)
    for k in range(1, n_ep):
        weight_copies[k - 1].wait_recv()
    wgot[me] = wsrc[me]
    tall = wgot.shape[2]
    spread = jnp.broadcast_to(wgot[...], (n_ep, seqs, tall))
    at_lane = lax.broadcasted_iota(jnp.int32, (n_ep, seqs, tall), 2)
    at_row = lax.broadcasted_iota(jnp.int32, (n_ep, seqs, tall), 1)
    column = jnp.sum(jnp.where(at_lane == at_row, spread, 0.0), axis=2, keepdims=True)
    column = column.reshape(n_ep * seqs, 1)
    loads[2].wait()
    loads[3].wait()
    loads[5].wait()
    loads[7].wait()
    scale_ref[...] = jnp.broadcast_to(column, (n_ep * seqs, 128))
    chunk = n_p * seqs
    crossing = {}
    returns = {}

    def rows_of(r):
        return pl.ds(pl.multiple_of((z + r) % n_z * chunk, chunk), chunk)

    def give_back(r):
        crossing[r].wait_recv()
        whole = (mine[r].astype(f32) + cross[r].astype(f32)).astype(bf16).astype(f32)
        weighted[r] = (whole * scale_ref[rows_of(r), 0:1]).astype(bf16)
        for k in range(1, n_p):
            to = (q + k) % n_p
            src = weighted.at[r, pl.ds(pl.multiple_of(to * seqs, seqs), seqs)]
            i = r * n_p + k
            returns[r, k] = send(src, plane_got.at[i], g_s.at[i], g_r.at[i], z * n_p + to, tp)

    arrival = [(n_z - d) % n_z for d in range(n_z)]
    for d in range(n_z):
        r = arrival[d]
        for k in range(1, n_p):
            plane[d, k].wait_recv()
            to_mate(d, k)
        for k in range(n_p):
            if d > 0 or k > 0:
                forwards[d, k].wait_recv()
        at = rows_of(r)
        left, right = rows[0, at], rows[1, at]
        gate = dot(left, egb[:half]) + dot(right, egb[half:])
        up = dot(left, eub[:half]) + dot(right, eub[half:])
        h = (silu(gate) * up).astype(bf16)
        other[r] = dot(h, edb[mate]).astype(bf16)
        crossing[r] = send(other.at[r], cross.at[r], x_s.at[r], x_r.at[r], me, mate)
        mine[r] = dot(h, edb[tp]).astype(bf16)
        if d > 0:
            give_back(arrival[d - 1])
    give_back(arrival[n_z - 1])
    mine_at = pl.ds(pl.multiple_of(q * seqs, seqs), seqs)
    lines = {}
    total = None
    for d in arrival[1:] + [0]:
        total = weighted[d, mine_at].astype(f32)
        for k in range(1, n_p):
            returns[d, k].wait_recv()
            total += plane_got[d * n_p + k].astype(f32)
        if d > 0:
            sums = line_send.at[d]
            line_send[d] = total.astype(bf16)
            lines[d] = send(
                sums, line_got.at[d], l_s.at[d], l_r.at[d], (z + d) % n_z * n_p + q, tp
            )
    shared_copy.wait_recv()
    shared = (shared_mine[...].astype(f32) + shared_got[...].astype(f32)).astype(bf16)
    for d in range(1, n_z):
        lines[d].wait_recv()
        total += line_got[d].astype(f32)
    out_ref[...] = (res[tp] + total + shared.astype(f32)).astype(bf16)
    everything = started + line[1:] + list(plane.values()) + list(forwards.values())
    everything += list(crossing.values()) + list(returns.values()) + list(lines.values())
    for c in everything + [shared_copy]:
        c.wait_send()


def local(n_ep, *args):
    (
        tokens, state, mix_gain, moe_gain, head_gain, w_forget, w_query, w_input, w_outgate,
        lower_bound, w_mix_out, routes, route_scores, expert_gate, expert_up, expert_down,
        shared_gate, shared_up, shared_down,
    ) = args
    seqs, width = tokens.shape
    heads, kdim, vdim = state.shape[1:]
    half = width // 2
    n_z = max(d for d in range(1, n_ep + 1) if d * d <= n_ep and n_ep % d == 0)
    n_p = n_ep // n_z
    experts = expert_gate.shape[0] * n_ep
    tall = -(-seqs // 128) * 128
    vmem = pl.BlockSpec(memory_space=pltpu.VMEM)
    anym = pl.BlockSpec(memory_space=pl.ANY)
    dma = pltpu.SemaphoreType.DMA
    inner = heads * vdim
    normed, readout, dense, new_state = pl.pallas_call(
        mixer_kernel,
        out_shape=(
            jax.ShapeDtypeStruct((seqs, width), bf16),
            jax.ShapeDtypeStruct((seqs, inner), f32),
            jax.ShapeDtypeStruct((experts, 1, tall), f32),
            jax.ShapeDtypeStruct(state.shape, f32),
        ),
        in_specs=[vmem] * 5 + [anym] * 4,
        out_specs=(vmem, vmem, vmem, anym),
        scratch_shapes=[
            pltpu.VMEM((3,) + w_forget.shape, bf16),
            pltpu.VMEM((heads, seqs, kdim, vdim), f32),
            pltpu.VMEM((heads, seqs, kdim, vdim), f32),
            dma((3,)),
            dma((heads,)),
            dma((heads,)),
        ],
        name="mixer",
    )(
        tokens, mix_gain.reshape(1, -1), lower_bound.reshape(1, -1), routes.T, route_scores.T,
        w_forget, w_input, w_query, state,
    )
    hid = expert_gate.shape[2]
    shid = shared_gate.shape[1]
    chunk = n_p * seqs
    layer_out = pl.pallas_call(
        functools.partial(moe_kernel, n_ep, n_z),
        out_shape=jax.ShapeDtypeStruct((seqs, half), bf16),
        in_specs=[vmem] * 6 + [anym] * 8,
        out_specs=vmem,
        scratch_shapes=[
            pltpu.VMEM(w_outgate.shape, bf16),
            pltpu.VMEM(w_mix_out.shape, bf16),
            pltpu.VMEM((seqs, inner), bf16),
            pltpu.VMEM((seqs, width), bf16),
            pltpu.VMEM((seqs, width), bf16),
            pltpu.VMEM((2, n_ep * seqs, half), bf16),
            pltpu.VMEM((2, seqs, half), f32),
            pltpu.VMEM((n_ep, 1, tall), f32),
            pltpu.VMEM((width, hid), bf16),
            pltpu.VMEM((width, hid), bf16),
            pltpu.VMEM((2, hid, half), bf16),
            pltpu.VMEM((width, shid), bf16),
            pltpu.VMEM((width, shid), bf16),
            pltpu.VMEM((2, shid, half), bf16),
            pltpu.VMEM((seqs, half), bf16),
            pltpu.VMEM((seqs, half), bf16),
            pltpu.VMEM((seqs, half), bf16),
            pltpu.VMEM((n_z, chunk, half), bf16),
            pltpu.VMEM((n_z, chunk, half), bf16),
            pltpu.VMEM((n_z, chunk, half), bf16),
            pltpu.VMEM((n_z, chunk, half), bf16),
            pltpu.VMEM((n_ep, seqs, half), bf16),
            pltpu.VMEM((n_z, seqs, half), bf16),
            pltpu.VMEM((n_z, seqs, half), bf16),
            pltpu.VMEM((n_ep * seqs, 128), f32),
            dma((10,)),
            dma((n_ep,)), dma((n_ep,)),
            dma, dma,
            dma((n_z,)), dma((n_z,)),
            dma((n_ep,)), dma((n_ep,)),
            dma((n_ep,)), dma((n_ep,)),
            dma, dma,
            dma((n_z,)), dma((n_z,)),
            dma((n_ep,)), dma((n_ep,)),
            dma((n_z,)), dma((n_z,)),
        ],
        compiler_params=pltpu.CompilerParams(collective_id=0, has_side_effects=True),
        name="experts",
    )(
        tokens, normed, readout, head_gain.reshape(1, -1), moe_gain.reshape(1, -1), dense,
        w_outgate, w_mix_out, expert_gate, expert_up, expert_down, shared_gate, shared_up, shared_down,
    )
    return (layer_out, new_state)


def solution(mesh):
    return jax.shard_map(
        functools.partial(local, mesh.shape["ep"]),
        mesh=mesh,
        in_specs=(
            P("ep", None),
            P("ep", "tp", None, None),
            P(),
            P(),
            P(),
            P(None, "tp"),
            P(None, "tp"),
            P(None, "tp"),
            P(None, "tp"),
            P("tp"),
            P("tp", None),
            P("ep", None),
            P("ep", None),
            P("ep", None, "tp"),
            P("ep", None, "tp"),
            P("ep", "tp", None),
            P(None, "tp"),
            P(None, "tp"),
            P("tp", None),
        ),
        out_specs=(P("ep", "tp"), P("ep", "tp", None, None)),
        check_vma=False,
    )
```

```python
import functools

import jax
import jax.numpy as jnp
from jax import lax
from jax.experimental import pallas as pl
from jax.experimental.pallas import tpu as pltpu
from jax.sharding import PartitionSpec as P

epsilon = 1e-06
routed_scale = 2.5
MESH = pl.DeviceIdType.MESH
f32 = jnp.float32
bf16 = jnp.bfloat16


def dot(a, b):
    return jnp.dot(a, b, preferred_element_type=f32)


def silu(v):
    return v * jax.nn.sigmoid(v)


def rms_scale(values, gain):
    return values * lax.rsqrt(jnp.mean(values * values, axis=-1, keepdims=True) + epsilon) * gain


def mixer_kernel(
    tok, gain, bound, routes, scores, wf, wi, wq, st,
    normed_out, readout, weights_out, new_st,
    wbuf, sbuf, nbuf, wsem, ssem, osem,
):
    seqs, heads, kdim, vdim = st.shape
    copies = [
        pltpu.make_async_copy(w, wbuf.at[i], wsem.at[i]) for i, w in enumerate((wf, wi, wq))
    ]
    state_copies = [
        pltpu.make_async_copy(st.at[:, h], sbuf.at[h], ssem.at[h]) for h in range(heads)
    ]
    for c in copies + state_copies:
        c.start()
    normed = rms_scale(tok[...].astype(f32), gain[...]).astype(bf16)
    normed_out[...] = normed

    score = scores[...]
    top = score.shape[0]
    weight = score / jnp.sum(score, axis=0, keepdims=True) * routed_scale
    named = routes[...]
    experts = weights_out.shape[0]
    number = lax.broadcasted_iota(jnp.int32, (experts, seqs), 0)
    dense = jnp.zeros((experts, seqs), f32)
    for t in range(top):
        dense += jnp.where(named[t : t + 1] == number, weight[t : t + 1], 0.0)
    tall = weights_out.shape[2]
    weights_out[:, 0, :] = jnp.concatenate([dense, jnp.zeros((experts, tall - seqs), f32)], axis=1)

    copies[0].wait()
    forget_pre = dot(normed, wbuf[0])
    low = bound[...]
    forget = low + (1.0 - low) * jax.nn.sigmoid(forget_pre)
    copies[1].wait()
    value = dot(normed, wbuf[1])
    copies[2].wait()
    query = silu(dot(normed, wbuf[2]))
    outs = []
    for h in range(heads):
        cols = slice(h * kdim, (h + 1) * kdim)
        vcols = slice(h * vdim, (h + 1) * vdim)
        ft, qt = forget[:, cols].T, query[:, cols].T
        vh = value[:, vcols]
        state_copies[h].wait()
        for s in range(seqs):
            row = vh[s : s + 1]
            new = row + ft[:, s : s + 1] * (sbuf[h, s] - row)
            nbuf[h, s] = new
            readout[s : s + 1, vcols] = jnp.sum(new * qt[:, s : s + 1], axis=0, keepdims=True)
        out = pltpu.make_async_copy(nbuf.at[h], new_st.at[:, h], osem.at[h])
        out.start()
        outs.append(out)
    for out in outs:
        out.wait()


def moe_kernel(
    n_ep, n_z, tok, mixer_in, readout, head_gain, gain, wsrc, wg, wm, eg, eu, ed, sg, su, sd,
    out_ref,
    wgb, wmb, gated, part_in, peer_part, rows, res, wgot, egb, eub, edb, sgb, sub, sdb,
    shared_send, shared_got, shared_mine, other, mine, cross, weighted, plane_got, line_send, line_got, scale_ref,
    wsem, bar_v_s, bar_v_r, ps_s, ps_r, a1_s, a1_r, a2_s, a2_r, fw_s, fw_r,
    sh_s, sh_r, x_s, x_r, g_s, g_r, l_s, l_r,
):
    n_p = n_ep // n_z
    me = lax.axis_index("ep")
    tp = lax.axis_index("tp")
    mate = 1 - tp
    z = me // n_p
    q = me % n_p
    seqs, width = tok.shape
    half = width // 2
    barrier = pltpu.get_barrier_semaphore()
    pl.semaphore_signal(barrier, inc=1, device_id=(me, mate), device_id_type=MESH)
    for k in range(1, n_ep):
        pl.semaphore_signal(
            barrier, inc=1, device_id=((me + k) % n_ep, tp), device_id_type=MESH
        )
    gate_load = pltpu.make_async_copy(wg, wgb, wsem.at[8])
    mix_load = pltpu.make_async_copy(wm, wmb, wsem.at[9])
    gate_load.start()
    mix_load.start()
    loads = []
    pairs = [(sg, sgb), (su, sub), (eg.at[0], egb), (eu.at[0], eub)]
    for i, (src, dst) in enumerate(pairs):
        loads.append(pltpu.make_async_copy(src, dst, wsem.at[i]))
    for c in range(2):
        loads.append(
            pltpu.make_async_copy(sd.at[:, pl.ds(c * half, half)], sdb.at[c], wsem.at[4 + c])
        )
        loads.append(
            pltpu.make_async_copy(ed.at[0, :, pl.ds(c * half, half)], edb.at[c], wsem.at[6 + c])
        )
    for c in loads:
        c.start()
    gate_load.wait()
    open_gate = silu(dot(mixer_in[...], wgb[...]))
    vdim = head_gain.shape[1]
    for h in range(readout.shape[1] // vdim):
        vcols = slice(h * vdim, (h + 1) * vdim)
        gated[:, vcols] = (
            rms_scale(readout[:, vcols], head_gain[...]) * open_gate[:, vcols]
        ).astype(bf16)
    mix_load.wait()
    part_in[...] = dot(gated[...], wmb[...]).astype(bf16)
    pl.semaphore_wait(barrier, n_ep)

    def send(src, dst, s, r, ep, core):
        c = pltpu.make_async_remote_copy(
            src_ref=src, dst_ref=dst, send_sem=s, recv_sem=r,
            device_id=(ep, core), device_id_type=MESH,
        )
        c.start()
        return c

    started = []
    psum = send(part_in, peer_part, ps_s, ps_r, me, mate)
    for k in range(1, n_ep):
        to = (me + k) % n_ep
        started.append(send(wsrc.at[to], wgot.at[me], bar_v_s.at[k], bar_v_r.at[k], to, tp))
    weight_copies = started[:]
    psum.wait()
    mixed = (part_in[...].astype(f32) + peer_part[...].astype(f32)).astype(bf16)
    residual = tok[...].astype(f32) + mixed.astype(f32)
    normed = rms_scale(residual, gain[...]).astype(bf16)
    own = pl.ds(pl.multiple_of(me * seqs, seqs), seqs)
    for c in range(2):
        cols = slice(c * half, (c + 1) * half)
        rows[c, own] = normed[:, cols]
        res[c] = residual[:, cols]

    def block(j):
        return rows.at[tp, pl.ds(pl.multiple_of(j * seqs, seqs), seqs)]

    line = [None]
    for d in range(1, n_z):
        to = (z + d) % n_z * n_p + q
        line.append(send(block(me), block(me), a1_s.at[d], a1_r.at[d], to, tp))
    plane = {}

    def to_plane(d):
        j = (z + n_z - d) % n_z * n_p + q
        for k in range(1, n_p):
            to = z * n_p + (q + k) % n_p
            plane[d, k] = send(
                block(j), block(j), a2_s.at[d * n_p + k], a2_r.at[d * n_p + k], to, tp
            )

    forwards = {}

    def to_mate(d, k):
        j = (z + n_z - d) % n_z * n_p + (q + n_p - k) % n_p
        i = d * n_p + k
        forwards[d, k] = send(block(j), block(j), fw_s.at[i], fw_r.at[i], me, mate)

    to_plane(0)

    loads[0].wait()
    loads[1].wait()
    shared_hidden = (silu(dot(normed, sgb[...])) * dot(normed, sub[...])).astype(bf16)
    loads[4].wait()
    loads[6].wait()
    shared_send[...] = dot(shared_hidden, sdb[mate]).astype(bf16)
    shared_copy = send(shared_send, shared_got, sh_s, sh_r, me, mate)
    shared_mine[...] = dot(shared_hidden, sdb[tp]).astype(bf16)

    for d in range(1, n_z):
        line[d].wait_recv()
        to_plane(d)
        to_mate(d, 0)
    for k in range(1, n_ep):
        weight_copies[k - 1].wait_recv()
    wgot[me] = wsrc[me]
    tall = wgot.shape[2]
    spread = jnp.broadcast_to(wgot[...], (n_ep, seqs, tall))
    at_lane = lax.broadcasted_iota(jnp.int32, (n_ep, seqs, tall), 2)
    at_row = lax.broadcasted_iota(jnp.int32, (n_ep, seqs, tall), 1)
    column = jnp.sum(jnp.where(at_lane == at_row, spread, 0.0), axis=2, keepdims=True)
    column = column.reshape(n_ep * seqs, 1)
    loads[2].wait()
    loads[3].wait()
    loads[5].wait()
    loads[7].wait()
    scale_ref[...] = jnp.broadcast_to(column, (n_ep * seqs, 128))
    chunk = n_p * seqs
    crossing = {}
    returns = {}

    def rows_of(r):
        return pl.ds(pl.multiple_of((z + r) % n_z * chunk, chunk), chunk)

    def give_back(r):
        crossing[r].wait_recv()
        whole = (mine[r].astype(f32) + cross[r].astype(f32)).astype(bf16).astype(f32)
        weighted[r] = (whole * scale_ref[rows_of(r), 0:1]).astype(bf16)
        for k in range(1, n_p):
            to = (q + k) % n_p
            src = weighted.at[r, pl.ds(pl.multiple_of(to * seqs, seqs), seqs)]
            i = r * n_p + k
            returns[r, k] = send(src, plane_got.at[i], g_s.at[i], g_r.at[i], z * n_p + to, tp)

    arrival = [(n_z - d) % n_z for d in range(n_z)]
    for d in range(n_z):
        r = arrival[d]
        for k in range(1, n_p):
            plane[d, k].wait_recv()
            to_mate(d, k)
        for k in range(n_p):
            if d > 0 or k > 0:
                forwards[d, k].wait_recv()
        at = rows_of(r)
        left, right = rows[0, at], rows[1, at]
        gate = dot(left, egb[:half]) + dot(right, egb[half:])
        up = dot(left, eub[:half]) + dot(right, eub[half:])
        h = (silu(gate) * up).astype(bf16)
        other[r] = dot(h, edb[mate]).astype(bf16)
        crossing[r] = send(other.at[r], cross.at[r], x_s.at[r], x_r.at[r], me, mate)
        mine[r] = dot(h, edb[tp]).astype(bf16)
        if d > 0:
            give_back(arrival[d - 1])
    give_back(arrival[n_z - 1])
    mine_at = pl.ds(pl.multiple_of(q * seqs, seqs), seqs)
    lines = {}
    total = None
    for d in arrival[1:] + [0]:
        total = weighted[d, mine_at].astype(f32)
        for k in range(1, n_p):
            returns[d, k].wait_recv()
            total += plane_got[d * n_p + k].astype(f32)
        if d > 0:
            sums = line_send.at[d]
            line_send[d] = total.astype(bf16)
            lines[d] = send(
                sums, line_got.at[d], l_s.at[d], l_r.at[d], (z + d) % n_z * n_p + q, tp
            )
    shared_copy.wait_recv()
    shared = (shared_mine[...].astype(f32) + shared_got[...].astype(f32)).astype(bf16)
    for d in range(1, n_z):
        lines[d].wait_recv()
        total += line_got[d].astype(f32)
    out_ref[...] = (res[tp] + total + shared.astype(f32)).astype(bf16)
    everything = started + line[1:] + list(plane.values()) + list(forwards.values())
    everything += list(crossing.values()) + list(returns.values()) + list(lines.values())
    for c in everything + [shared_copy]:
        c.wait_send()


def local(n_ep, *args):
    (
        tokens, state, mix_gain, moe_gain, head_gain, w_forget, w_query, w_input, w_outgate,
        lower_bound, w_mix_out, routes, route_scores, expert_gate, expert_up, expert_down,
        shared_gate, shared_up, shared_down,
    ) = args
    seqs, width = tokens.shape
    heads, kdim, vdim = state.shape[1:]
    half = width // 2
    n_z = max(d for d in range(1, n_ep + 1) if d * d <= n_ep and n_ep % d == 0)
    n_p = n_ep // n_z
    experts = expert_gate.shape[0] * n_ep
    tall = -(-seqs // 128) * 128
    vmem = pl.BlockSpec(memory_space=pltpu.VMEM)
    anym = pl.BlockSpec(memory_space=pl.ANY)
    dma = pltpu.SemaphoreType.DMA
    inner = heads * vdim
    normed, readout, dense, new_state = pl.pallas_call(
        mixer_kernel,
        out_shape=(
            jax.ShapeDtypeStruct((seqs, width), bf16),
            jax.ShapeDtypeStruct((seqs, inner), f32),
            jax.ShapeDtypeStruct((experts, 1, tall), f32),
            jax.ShapeDtypeStruct(state.shape, f32),
        ),
        in_specs=[vmem] * 5 + [anym] * 4,
        out_specs=(vmem, vmem, vmem, anym),
        scratch_shapes=[
            pltpu.VMEM((3,) + w_forget.shape, bf16),
            pltpu.VMEM((heads, seqs, kdim, vdim), f32),
            pltpu.VMEM((heads, seqs, kdim, vdim), f32),
            dma((3,)),
            dma((heads,)),
            dma((heads,)),
        ],
        name="mixer",
    )(
        tokens, mix_gain.reshape(1, -1), lower_bound.reshape(1, -1), routes.T, route_scores.T,
        w_forget, w_input, w_query, state,
    )
    hid = expert_gate.shape[2]
    shid = shared_gate.shape[1]
    chunk = n_p * seqs
    layer_out = pl.pallas_call(
        functools.partial(moe_kernel, n_ep, n_z),
        out_shape=jax.ShapeDtypeStruct((seqs, half), bf16),
        in_specs=[vmem] * 6 + [anym] * 8,
        out_specs=vmem,
        scratch_shapes=[
            pltpu.VMEM(w_outgate.shape, bf16),
            pltpu.VMEM(w_mix_out.shape, bf16),
            pltpu.VMEM((seqs, inner), bf16),
            pltpu.VMEM((seqs, width), bf16),
            pltpu.VMEM((seqs, width), bf16),
            pltpu.VMEM((2, n_ep * seqs, half), bf16),
            pltpu.VMEM((2, seqs, half), f32),
            pltpu.VMEM((n_ep, 1, tall), f32),
            pltpu.VMEM((width, hid), bf16),
            pltpu.VMEM((width, hid), bf16),
            pltpu.VMEM((2, hid, half), bf16),
            pltpu.VMEM((width, shid), bf16),
            pltpu.VMEM((width, shid), bf16),
            pltpu.VMEM((2, shid, half), bf16),
            pltpu.VMEM((seqs, half), bf16),
            pltpu.VMEM((seqs, half), bf16),
            pltpu.VMEM((seqs, half), bf16),
            pltpu.VMEM((n_z, chunk, half), bf16),
            pltpu.VMEM((n_z, chunk, half), bf16),
            pltpu.VMEM((n_z, chunk, half), bf16),
            pltpu.VMEM((n_z, chunk, half), bf16),
            pltpu.VMEM((n_ep, seqs, half), bf16),
            pltpu.VMEM((n_z, seqs, half), bf16),
            pltpu.VMEM((n_z, seqs, half), bf16),
            pltpu.VMEM((n_ep * seqs, 128), f32),
            dma((10,)),
            dma((n_ep,)), dma((n_ep,)),
            dma, dma,
            dma((n_z,)), dma((n_z,)),
            dma((n_ep,)), dma((n_ep,)),
            dma((n_ep,)), dma((n_ep,)),
            dma, dma,
            dma((n_z,)), dma((n_z,)),
            dma((n_ep,)), dma((n_ep,)),
            dma((n_z,)), dma((n_z,)),
        ],
        compiler_params=pltpu.CompilerParams(collective_id=0, has_side_effects=True),
        name="experts",
    )(
        tokens, normed, readout, head_gain.reshape(1, -1), moe_gain.reshape(1, -1), dense,
        w_outgate, w_mix_out, expert_gate, expert_up, expert_down, shared_gate, shared_up, shared_down,
    )
    return (layer_out, new_state)


def solution(mesh):
    return jax.shard_map(
        functools.partial(local, mesh.shape["ep"]),
        mesh=mesh,
        in_specs=(
            P("ep", None),
            P("ep", "tp", None, None),
            P(),
            P(),
            P(),
            P(None, "tp"),
            P(None, "tp"),
            P(None, "tp"),
            P(None, "tp"),
            P("tp"),
            P("tp", None),
            P("ep", None),
            P("ep", None),
            P("ep", None, "tp"),
            P("ep", None, "tp"),
            P("ep", "tp", None),
            P(None, "tp"),
            P(None, "tp"),
            P("tp", None),
        ),
        out_specs=(P("ep", "tp"), P("ep", "tp", None, None)),
        check_vma=False,
    )
```
